32 devices in a mesh: fs: 8 (over z, core), tp: 4 (over y, x).
Axes of the slice: x: 2, y: 2, z: 4, core: 2. Of those that a mesh axis runs over, the one named last changes fastest.
Arguments:
- normed_in: bfloat16 [8192, 2048], P('fs'), may hold values from -6 to 6
- grad_x: bfloat16 [8192, 2048], P('fs', 'tp'), may hold values from -0.088388348 to 0.088388348
- grad_y: bfloat16 [8192, 2048], P('fs', 'tp'), may hold values from -0.088388348 to 0.088388348
- weight_x: float32 [2048, 2048], P('fs', 'tp'), may hold values from -0.125 to 0.125
- weight_y: float32 [2048, 2048], P('fs', 'tp'), may hold values from -0.125 to 0.125
- factor_x: bfloat16 [2048, 512], P('fs'), may hold values from -0.13258252 to 0.13258252
- factor_y: bfloat16 [2048, 512], P('fs'), may hold values from -0.13258252 to 0.13258252
- first_x: float32 [512, 2048], P('fs', 'tp'), may hold values from -8 to 8
- first_y: float32 [512, 2048], P('fs', 'tp'), may hold values from -8 to 8
- second_x: float32 [512, 2048], P('fs', 'tp'), may hold values from 0.5 to 2
- second_y: float32 [512, 2048], P('fs', 'tp'), may hold values from 0.5 to 2
Outputs:
- new_weight_x: float32 [2048, 2048], P('fs', 'tp')
- new_weight_y: float32 [2048, 2048], P('fs', 'tp')
- step_x: float32 [2048, 2048], P('fs', 'tp')
- step_y: float32 [2048, 2048], P('fs', 'tp')
- new_first_x: float32 [512, 2048], P('fs', 'tp')
- new_first_y: float32 [512, 2048], P('fs', 'tp')
- new_second_x: float32 [512, 2048], P('fs', 'tp')
- new_second_y: float32 [512, 2048], P('fs', 'tp')
- copy_x: bfloat16 [2048, 2048], P(None, 'tp')
- copy_y: bfloat16 [2048, 2048], P(None, 'tp')
The draws below stay inside these ranges and needn't reach their ends.
All inputs are finite; a program needn't handle non-finite values.
Results may differ from the reference program's by a relative error of at most 0.02.
Values may be sent and summed in bfloat16 or wider, within the bound.
A program may use at most 128 MiB of HBM per device.

```python
import math
import jax
import jax.numpy as jnp
from jax import lax

D = 2048
RW = 2048
RANK = 512
TOKENS = 8192


def noise_block(key, shape):
    return jnp.clip(jax.random.normal(key, shape, jnp.float32), -6.0, 6.0)


def bounded_normal(key, shape):
    return jnp.clip(jax.random.normal(key, shape, jnp.float32), -3.0, 3.0)


def token_scales(key):
    return bounded_normal(jax.random.fold_in(key, 101), (TOKENS,))


def draw_normed_in(key, part):
    feature = bounded_normal(jax.random.fold_in(key, 102), (D,))
    background = noise_block(jax.random.fold_in(key, 103), (TOKENS, D))
    mixed = background + 0.5 * token_scales(key)[:, None] * feature[None, :]
    return jnp.clip(mixed, -6.0, 6.0).astype(jnp.bfloat16)


def cotangent_draw(key, tag):
    strength = 12.0
    channel = bounded_normal(jax.random.fold_in(key, tag), (RW,))
    background = noise_block(jax.random.fold_in(key, tag + 1), (TOKENS, RW)) * TOKENS ** (-0.5)
    coherent = strength / TOKENS * token_scales(key)[:, None] * channel[None, :]
    ceiling = 8.0 * TOKENS ** (-0.5)
    return jnp.clip(background + coherent, -ceiling, ceiling).astype(jnp.bfloat16)


def draw_grad_x(key, part):
    return cotangent_draw(key, 201)


def draw_grad_y(key, part):
    return cotangent_draw(key, 211)


def factor_draw(key, tag):
    shared_weight = 0.1
    common = bounded_normal(jax.random.fold_in(key, tag), (D,))
    spread_block = noise_block(jax.random.fold_in(key, tag + 1), (D, RANK))
    ceiling = 6.0 * D ** (-0.5)
    factor = (spread_block + shared_weight * common[:, None]) * D ** (-0.5)
    return jnp.clip(factor, -ceiling, ceiling).astype(jnp.bfloat16)


def draw_factor_x(key, part):
    return factor_draw(key, 301)


def draw_factor_y(key, part):
    return factor_draw(key, 311)


def moment_draw(key, tag):
    column_mean = bounded_normal(jax.random.fold_in(key, tag), (RW,))
    ripple = noise_block(jax.random.fold_in(key, tag + 1), (RANK, RW))
    return jnp.clip(ripple + column_mean[None, :], -8.0, 8.0)


def draw_first_x(key, part):
    return moment_draw(key, 401)


def draw_first_y(key, part):
    return moment_draw(key, 411)


def level_of(rng, shape, split, least, top_value):
    level, own = 1.0, jax.random.fold_in(rng, 6)
    for position, parts in split:
        draws = jnp.exp(jax.random.uniform(jax.random.fold_in(own, position), (parts,), jnp.float32, least / len(split), top_value / len(split)))
        level = level * jnp.repeat(draws, shape[position] // parts).reshape([-1 if axis == position else 1 for axis in range(len(shape))])
    return level


def gaussian(stream_key, shape, deviation, bound, split=(), dtype=jnp.bfloat16):
    array = deviation * jax.random.normal(stream_key, shape, jnp.float32)
    if split:
        array = array * level_of(stream_key, shape, split, -0.22, 0.18)
    return jnp.clip(array, -bound, bound).astype(dtype)


def setup_inputs(seed: int = 0) -> dict:
    key_of = jax.random.split(jax.random.key(seed), 12)
    normed_in = draw_normed_in(jax.random.fold_in(key_of[11], 71), 0)
    grad_x = draw_grad_x(jax.random.fold_in(key_of[11], 71), 0)
    grad_y = draw_grad_y(jax.random.fold_in(key_of[11], 71), 0)
    weight_x = gaussian(key_of[3], (D, RW), D ** -0.5, 0.125, ((0, 8), (1, 4)), jnp.float32)
    weight_y = gaussian(key_of[4], (D, RW), D ** -0.5, 0.125, ((0, 8), (1, 4)), jnp.float32)
    factor_x = draw_factor_x(jax.random.fold_in(key_of[11], 71), 0)
    factor_y = draw_factor_y(jax.random.fold_in(key_of[11], 71), 0)
    first_x = draw_first_x(jax.random.fold_in(key_of[11], 71), 0)
    first_y = draw_first_y(jax.random.fold_in(key_of[11], 71), 0)
    second_x = jnp.clip(jnp.exp(math.log(2.0) - 1.3862944 * jax.random.uniform(key_of[9], (RANK, RW), jnp.float32) ** level_of(key_of[9], (RANK, RW), ((0, 8), (1, 4)), -0.2, 0.2)), 0.5, 2.0)
    second_y = jnp.clip(jnp.exp(math.log(2.0) - 1.3862944 * jax.random.uniform(key_of[10], (RANK, RW), jnp.float32) ** level_of(key_of[10], (RANK, RW), ((0, 8), (1, 4)), -0.2, 0.2)), 0.5, 2.0)
    return {"normed_in": normed_in, "grad_x": grad_x, "grad_y": grad_y, "weight_x": weight_x, "weight_y": weight_y, "factor_x": factor_x, "factor_y": factor_y, "first_x": first_x, "first_y": first_y, "second_x": second_x, "second_y": second_y}


def branch(normed_in, cotangent, factor, first, second):
    gradient = lax.dot_general(normed_in, cotangent, (((0,), (0,)), ((), ())), preferred_element_type=jnp.float32)
    factor_full = factor.astype(jnp.float32)
    low = jnp.dot(factor_full.T, gradient, precision=lax.Precision.HIGHEST)
    first_new = 0.8 * first + 0.2 * low
    second_new = 0.9 * second + 0.1 * low * low
    direction = first_new / jnp.sqrt(second_new)
    update = jnp.dot(factor_full, direction, precision=lax.Precision.HIGHEST)
    return (update, first_new, second_new)

def reference(normed_in, grad_x, grad_y, weight_x, weight_y, factor_x, factor_y, first_x, first_y, second_x, second_y):
    update_x, first_new_x, second_new_x = branch(normed_in, grad_x, factor_x, first_x, second_x)
    update_y, first_new_y, second_new_y = branch(normed_in, grad_y, factor_y, first_y, second_y)
    total = jnp.sum(update_x * update_x) + jnp.sum(update_y * update_y)
    scale = jnp.minimum(1.0, 0.25 * jnp.sqrt(2.0 * D * RW) / jnp.sqrt(total))
    step_x = scale * update_x
    step_y = scale * update_y
    new_x = weight_x - 0.02 * step_x
    new_y = weight_y - 0.02 * step_y
    return (new_x, new_y, step_x, step_y, first_new_x, first_new_y, second_new_x, second_new_y, new_x.astype(jnp.bfloat16), new_y.astype(jnp.bfloat16))
```

```python
import functools
import math

import jax
import jax.numpy as jnp
from jax import lax
from jax.experimental import pallas as pl
from jax.experimental.pallas import tpu as pltpu
from jax.sharding import PartitionSpec as P

MESH = pl.DeviceIdType.MESH
F32, BF16 = jnp.float32, jnp.bfloat16
ROWS = (((0,), (0,)), ((), ()))


def exchange_kernel(
    nfs,
    ntp,
    normed,
    grad_x,
    grad_y,
    weight_x,
    weight_y,
    factor_x,
    factor_y,
    first_x,
    first_y,
    second_x,
    second_y,
    f_out,
    w_out,
    d_out,
    low_out,
    tot_out,
    n_buf,
    gx_buf,
    gy_buf,
    f_buf,
    h_buf,
    low,
    sib,
    rs_send,
    rs_recv,
    d_buf,
    w_buf,
    w16,
    fm,
    sm,
    g_hi,
    g_lo,
    tot_recv,
    lsem,
    bar_sem,
    f_line_s,
    f_line_r,
    f_tp_s,
    f_tp_r,
    f_sib_s,
    f_sib_r,
    f_own_s,
    w_s,
    w_r,
    w_sib_s,
    w_sib_r,
    sib_s,
    rs_s,
    rs_r,
    d_line_s,
    d_line_r,
    d_sib_s,
    d_sib_r,
    t_s,
    t_r,
):
    nz = nfs // 2
    i = lax.axis_index("fs")
    t = lax.axis_index("tp")
    z, c = i // 2, lax.rem(i, 2)
    o = z * 2 + 1 - c
    R, rank = factor_x.shape
    tokens, w = gx_buf.shape
    r = rank // nfs
    q = math.gcd(ntp, R // 16)
    rq = R // q
    u, g0 = lax.rem(t, q), t // q * q

    def local(src, dst, k):
        cp = pltpu.make_async_copy(src, dst, lsem.at[k])
        cp.start()
        return cp

    def send(src, dst, s, rr, dev):
        return pltpu.make_async_remote_copy(
            src_ref=src, dst_ref=dst, send_sem=s, recv_sem=rr, device_id=dev, device_id_type=MESH
        )

    def rows(k, n):
        return pl.ds(pl.multiple_of(k * n, n), n)

    cps_f = [
        local(factor_x, f_buf.at[0, rows(i, R)], 0),
        local(factor_y, f_buf.at[1, rows(i, R)], 1),
    ]
    cps_w = [
        local(weight_x, w_buf.at[:, pl.ds(0, w)], 2),
        local(weight_y, w_buf.at[:, pl.ds(w, w)], 3),
    ]
    cps_n = [local(normed, n_buf, 4), local(grad_x, gx_buf, 5), local(grad_y, gy_buf, 6)]
    cps_m = [
        local(first_x, fm.at[:, pl.ds(0, w)], 7),
        local(first_y, fm.at[:, pl.ds(w, w)], 8),
        local(second_x, sm.at[:, pl.ds(0, w)], 9),
        local(second_y, sm.at[:, pl.ds(w, w)], 10),
    ]

    barrier = pltpu.get_barrier_semaphore()
    peers = [{"fs": lax.rem(z + k, nz) * 2 + c} for k in range(1, nz)] + [{"fs": o}]
    peers += [{"tp": lax.rem(t + k, ntp)} for k in range(1, ntp)]
    for dev in peers:
        pl.semaphore_signal(barrier, inc=1, device_id=dev, device_id_type=MESH)
    pl.semaphore_wait(barrier, len(peers))
    for cp in cps_f:
        cp.wait()

    sent = []

    def go(cp):
        cp.start()
        sent.append(cp)

    def piece(src_fs, part):
        return f_buf.at[:, pl.ds(pl.multiple_of(src_fs * R + part * rq, rq), rq)]

    own = piece(i, u)
    for k in range(1, nz):
        zd = lax.rem(z + k, nz)
        go(send(own, own, f_line_s.at[k], f_line_r.at[z], {"fs": zd * 2 + c}))
    mine = f_buf.at[:, rows(i, R)]
    go(send(mine, mine, f_own_s.at[0], f_sib_r.at[z, 0], {"fs": o}))

    for cp in cps_w:
        cp.wait()
    w16[...] = w_buf[...].astype(BF16)
    put = local(w16, w_out.at[rows(i, R)], 2)

    def w_hop(step):
        for side, sign in ((0, 1), (1, -1)):
            src = z - sign * step
            nxt = z + sign
            has = (src >= 0) & (src < nz)
            to = has & (nxt >= 0) & (nxt < nz)
            slot = w_out.at[rows(src * 2 + c, R)]

            if step:

                @pl.when(has)
                def _():
                    send(slot, slot, w_s.at[0, side], w_r.at[src], {"fs": o}).wait_recv()
                    send(slot, slot, w_sib_s.at[src], w_sib_r.at[src], {"fs": o}).start()

            @pl.when(to)
            def _():
                a = slot if step else w16
                send(a, slot, w_s.at[step, side], w_r.at[src], {"fs": nxt * 2 + c}).start()

    w_hop(0)
    w_own = w_out.at[rows(i, R)]
    go(send(w16, w_own, w_sib_s.at[z], w_sib_r.at[z], {"fs": o}))

    for k in range(1, nz):
        zs = lax.rem(z + nz - k, nz)
        p = piece(zs * 2 + c, u)
        send(p, p, f_line_s.at[k], f_line_r.at[zs], {"fs": o}).wait_recv()
        for v in range(1, q):
            go(send(p, p, f_tp_s.at[zs, v], f_tp_r.at[zs, u], {"tp": g0 + lax.rem(u + v, q)}))
        go(send(p, p, f_sib_s.at[zs, 0], f_sib_r.at[zs, u], {"fs": o}))
    for k in range(1, nz):
        zs = lax.rem(z + nz - k, nz)
        for v in range(1, q):
            part = lax.rem(u + v, q)
            p = piece(zs * 2 + c, part)
            send(p, p, f_tp_s.at[zs, v], f_tp_r.at[zs, part], {"fs": o}).wait_recv()
            go(send(p, p, f_sib_s.at[zs, v], f_sib_r.at[zs, part], {"fs": o}))
    theirs = f_buf.at[:, rows(o, R)]
    send(theirs, theirs, f_own_s.at[0], f_sib_r.at[z, 0], {"fs": o}).wait_recv()
    for k in range(1, nz):
        zs = lax.rem(z + nz - k, nz)
        for v in range(q):
            p = piece(zs * 2 + 1 - c, v)
            send(p, p, f_sib_s.at[zs, v], f_sib_r.at[zs, v], {"fs": o}).wait_recv()
    keep_f = local(f_buf, f_out, 0)

    for cp in cps_n:
        cp.wait()
    tile = min(256, tokens)

    @pl.loop(0, tokens // tile)
    def _(k):
        a = n_buf[rows(k, tile), :]
        for b in range(2):
            h = jnp.dot(a, f_buf[b], preferred_element_type=F32)
            h_buf[rows(k, tile), pl.ds(b * rank, rank)] = h.astype(BF16)

    lanes = 128
    m = lanes // (2 * r)

    @pl.loop(0, rank // lanes)
    def _(k):
        for b, g in ((0, gx_buf), (1, gy_buf)):
            h = h_buf[:, pl.ds(pl.multiple_of(b * rank + k * lanes, lanes), lanes)]
            part = lax.dot_general(h, g[...], ROWS, preferred_element_type=F32)
            low[pl.ds(k * m, m), :, :, pl.ds(b * w, w)] = part.reshape(m, 2, r, w)

    go(send(low.at[:, 1 - c], sib, sib_s.at[0], sib_s.at[1], {"fs": o}))
    sent[-1].wait_recv()
    for k in range(1, nz):
        zd = lax.rem(z + k, nz)
        rs_send[zd] = (low[zd, c] + sib[zd]).astype(BF16)
        go(send(rs_send.at[zd], rs_recv.at[z], rs_s.at[k], rs_r.at[z], {"fs": zd * 2 + c}))

    for step in range(1, nz - 1):
        w_hop(step)

    @pl.loop(0, rank // lanes)
    def _(k):
        for b in range(2):
            cols = pl.ds(pl.multiple_of(k * lanes, lanes), lanes)
            gram = lax.dot_general(f_buf[b, :, cols], f_buf[b], ROWS, preferred_element_type=F32)
            hi = gram.astype(BF16)
            g_hi[b, rows(k, lanes), :] = hi
            g_lo[b, rows(k, lanes), :] = (gram - hi.astype(F32)).astype(BF16)

    for cp in cps_m:
        cp.wait()
    total = low[z, c] + sib[z]
    for k in range(1, nz):
        zs = lax.rem(z + k, nz)
        send(rs_recv.at[zs], rs_recv.at[zs], rs_s.at[k], rs_r.at[zs], {"fs": o}).wait_recv()
        total = total + rs_recv[zs].astype(F32)
    low_out[...] = total
    nf = 0.8 * fm[...] + 0.2 * total
    ns = 0.9 * sm[...] + 0.1 * total * total
    d_buf[rows(i, r), :] = (nf / jnp.sqrt(ns)).astype(BF16)

    d_own = d_buf.at[rows(i, r)]
    for k in range(1, nz):
        zd = lax.rem(z + k, nz)
        go(send(d_own, d_own, d_line_s.at[k], d_line_r.at[z], {"fs": zd * 2 + c}))
    go(send(d_own, d_own, d_sib_s.at[z], d_sib_r.at[z], {"fs": o}))
    for k in range(1, nz):
        zs = lax.rem(z + k, nz)
        p = d_buf.at[rows(zs * 2 + c, r)]
        send(p, p, d_line_s.at[k], d_line_r.at[zs], {"fs": o}).wait_recv()
        go(send(p, p, d_sib_s.at[zs], d_sib_r.at[zs], {"fs": o}))
    for k in range(nz):
        zs = lax.rem(z + k, nz)
        p = d_buf.at[rows(zs * 2 + 1 - c, r)]
        send(p, p, d_sib_s.at[zs], d_sib_r.at[zs], {"fs": o}).wait_recv()
    keep_d = local(d_buf, d_out, 1)

    part = 0.0
    for b in range(2):
        d = d_buf[:, pl.ds(b * w, w)]
        gd = jnp.dot(g_hi[b], d, preferred_element_type=F32)
        gd = gd + jnp.dot(g_lo[b], d, preferred_element_type=F32)
        part = part + jnp.sum(gd * d.astype(F32))
    tot_recv[t] = jnp.full(tot_recv.shape[1:], part, F32)
    for k in range(1, ntp):
        slot = tot_recv.at[t]
        go(send(slot, slot, t_s.at[k], t_r.at[t], {"tp": lax.rem(t + k, ntp)}))

    if nz > 1:
        w_hop(nz - 1)

    acc = tot_recv[t]
    for k in range(1, ntp):
        ts = lax.rem(t + k, ntp)
        slot = tot_recv.at[ts]
        send(slot, slot, t_s.at[k], t_r.at[ts], {"fs": o}).wait_recv()
        acc = acc + tot_recv[ts]
    tot_out[...] = acc

    for zs in range(nz):
        slot = w_out.at[pl.ds((zs * 2) * R, R)]
        send(slot, slot, w_sib_s.at[zs], w_sib_r.at[zs], {"fs": o}).wait_recv()

        @pl.when(zs != z)
        def _():
            send(slot, slot, w_sib_s.at[zs], w_sib_r.at[zs], {"fs": o}).wait_send()

    for step in range(nz - 1):
        for side, sign in ((0, 1), (1, -1)):
            src = z - sign * step
            nxt = z + sign

            @pl.when((src >= 0) & (src < nz) & (nxt >= 0) & (nxt < nz))
            def _():
                a = w_out.at[rows(src * 2 + c, R)] if step else w16
                send(a, a, w_s.at[step, side], w_r.at[0], {"fs": o}).wait_send()

    for cp in sent:
        cp.wait_send()
    put.wait()
    keep_f.wait()
    keep_d.wait()


def output_kernel(
    scale_top,
    f_full,
    w_full,
    d,
    low,
    tot,
    weight_x,
    weight_y,
    factor_x,
    factor_y,
    first_x,
    first_y,
    second_x,
    second_y,
    new_x,
    new_y,
    step_x,
    step_y,
    nf_x,
    nf_y,
    ns_x,
    ns_y,
    copy_x,
    copy_y,
):
    scale = jnp.minimum(1.0, scale_top / jnp.sqrt(tot[0:1, 0:1]))
    w = weight_x.shape[1]
    sides = (
        (factor_x, weight_x, first_x, second_x, new_x, step_x, nf_x, ns_x, copy_x),
        (factor_y, weight_y, first_y, second_y, new_y, step_y, nf_y, ns_y, copy_y),
    )
    for b, (factor, weight, first, second, new, step, nf, ns, copy) in enumerate(sides):
        cols = pl.ds(b * w, w)
        db = d[:, cols]
        up = jnp.dot(f_full[b], db, preferred_element_type=F32)
        copy[...] = (w_full[:, cols].astype(F32) - 0.02 * (scale * up)).astype(BF16)
        st = scale * jnp.dot(factor[...], db, preferred_element_type=F32)
        step[...] = st
        new[...] = weight[...] - 0.02 * st

        @pl.when(pl.program_id(0) == 0)
        def _():
            lo = low[:, cols]
            nf[...] = 0.8 * first[...] + 0.2 * lo
            ns[...] = 0.9 * second[...] + 0.1 * lo * lo


def on_device(nfs, ntp, normed, gx, gy, wx, wy, fx, fy, mx, my, sx, sy):
    tokens, depth = normed.shape
    w = gx.shape[1]
    R, rank = fx.shape
    r = rank // nfs
    nz = nfs // 2
    q = math.gcd(ntp, R // 16)
    anyspec = pl.BlockSpec(memory_space=pl.ANY)
    vmem = pl.BlockSpec(memory_space=pltpu.VMEM)
    dma = pltpu.SemaphoreType.DMA
    sds = jax.ShapeDtypeStruct
    V = pltpu.VMEM
    f_full, w_full, d, low, tot = pl.pallas_call(
        functools.partial(exchange_kernel, nfs, ntp),
        out_shape=(
            sds((2, depth, rank), BF16),
            sds((depth, 2 * w), BF16),
            sds((rank, 2 * w), BF16),
            sds((r, 2 * w), F32),
            sds((8, 128), F32),
        ),
        in_specs=[anyspec] * 11,
        out_specs=(anyspec, anyspec, anyspec, vmem, vmem),
        scratch_shapes=[
            V((tokens, depth), BF16),
            V((tokens, w), BF16),
            V((tokens, w), BF16),
            V((2, depth, rank), BF16),
            V((tokens, 2 * rank), BF16),
            V((nz, 2, r, 2 * w), F32),
            V((nz, r, 2 * w), F32),
            V((nz, r, 2 * w), BF16),
            V((nz, r, 2 * w), BF16),
            V((rank, 2 * w), BF16),
            V((R, 2 * w), F32),
            V((R, 2 * w), BF16),
            V((r, 2 * w), F32),
            V((r, 2 * w), F32),
            V((2, rank, rank), BF16),
            V((2, rank, rank), BF16),
            V((ntp, 8, 128), F32),
            dma((11,)),
            pltpu.SemaphoreType.REGULAR,
            dma((nz,)),
            dma((nz,)),
            dma((nz, q)),
            dma((nz, q)),
            dma((nz, q)),
            dma((nz, q)),
            dma((1,)),
            dma((nz, 2)),
            dma((nz,)),
            dma((nz,)),
            dma((nz,)),
            dma((2,)),
            dma((nz,)),
            dma((nz,)),
            dma((nz,)),
            dma((nz,)),
            dma((nz,)),
            dma((nz,)),
            dma((ntp,)),
            dma((ntp,)),
        ],
        compiler_params=pltpu.CompilerParams(
            collective_id=0, has_side_effects=True, vmem_limit_bytes=56 * 1024 * 1024
        ),
    )(normed, gx, gy, wx, wy, fx, fy, mx, my, sx, sy)

    n = min(8, R // 16)
    big, small = depth // n, R // n

    def block(rows, cols):
        return pl.BlockSpec((rows, cols), lambda k: (k, 0))

    def whole(rows, cols):
        return pl.BlockSpec((rows, cols), lambda k: (0, 0))

    return pl.pallas_call(
        functools.partial(output_kernel, 0.25 * math.sqrt(2.0 * depth * w * ntp)),
        grid=(n,),
        out_shape=[sds((R, w), F32)] * 4 + [sds((r, w), F32)] * 4 + [sds((depth, w), BF16)] * 2,
        in_specs=[
            pl.BlockSpec((2, big, rank), lambda k: (0, k, 0)),
            block(big, 2 * w),
            whole(rank, 2 * w),
            whole(r, 2 * w),
            whole(8, 128),
        ]
        + [block(small, w)] * 2
        + [block(small, rank)] * 2
        + [whole(r, w)] * 4,
        out_specs=[block(small, w)] * 4 + [whole(r, w)] * 4 + [block(big, w)] * 2,
        compiler_params=pltpu.CompilerParams(vmem_limit_bytes=40 * 1024 * 1024),
    )(f_full, w_full, d, low, tot, wx, wy, fx, fy, mx, my, sx, sy)


def solution(mesh):
    row, cut, rep = P("fs", None), P("fs", "tp"), P(None, "tp")
    return jax.shard_map(
        functools.partial(on_device, mesh.shape["fs"], mesh.shape["tp"]),
        mesh=mesh,
        in_specs=(row, cut, cut, cut, cut, row, row, cut, cut, cut, cut),
        out_specs=(cut,) * 8 + (rep, rep),
        check_vma=False,
    )
```

```python
import functools
import math

import jax
import jax.numpy as jnp
from jax import lax
from jax.experimental import pallas as pl
from jax.experimental.pallas import tpu as pltpu
from jax.sharding import PartitionSpec as P

MESH = pl.DeviceIdType.MESH
F32, BF16 = jnp.float32, jnp.bfloat16
PLACE = {"h": ((1, 0),), "scatter": ((1, 1), (2, 0)), "dir": ((2, 1),), "end": (("rest", 3),)}
ROWS = (((0,), (0,)), ((), ()))


def exchange_kernel(
    nfs,
    ntp,
    normed,
    grad_x,
    grad_y,
    weight_x,
    weight_y,
    factor_x,
    factor_y,
    first_x,
    first_y,
    second_x,
    second_y,
    f_buf,
    w_out,
    d_buf,
    low_out,
    tot_out,
    n_buf,
    gx_buf,
    gy_buf,
    h_buf,
    low,
    sib,
    rs_send,
    rs_recv,
    w_buf,
    w16,
    fm,
    sm,
    g_hi,
    g_lo,
    tot_recv,
    lsem,
    f_line_s,
    f_line_r,
    f_tp_s,
    f_tp_r,
    f_sib_s,
    f_sib_r,
    f_own_s,
    w_s,
    w_r,
    w_sib_s,
    w_sib_r,
    sib_s,
    rs_s,
    rs_r,
    d_line_s,
    d_line_r,
    d_sib_s,
    d_sib_r,
    t_s,
    t_r,
):
    nz = nfs // 2
    i = lax.axis_index("fs")
    t = lax.axis_index("tp")
    z, c = i // 2, lax.rem(i, 2)
    o = z * 2 + 1 - c
    R, rank = factor_x.shape
    tokens, w = gx_buf.shape
    r = rank // nfs
    q = math.gcd(ntp, R // 16)
    rq = R // q
    u, g0 = lax.rem(t, q), t // q * q

    def local(src, dst, k):
        cp = pltpu.make_async_copy(src, dst, lsem.at[k])
        cp.start()
        return cp

    def send(src, dst, s, rr, dev):
        return pltpu.make_async_remote_copy(
            src_ref=src, dst_ref=dst, send_sem=s, recv_sem=rr, device_id=dev, device_id_type=MESH
        )

    def rows(k, n):
        return pl.ds(pl.multiple_of(k * n, n), n)

    cps_f = [
        local(factor_x, f_buf.at[0, rows(i, R)], 0),
        local(factor_y, f_buf.at[1, rows(i, R)], 1),
    ]
    cps_w = [
        local(weight_x, w_buf.at[:, pl.ds(0, w)], 2),
        local(weight_y, w_buf.at[:, pl.ds(w, w)], 3),
    ]
    cps_n = [local(normed, n_buf, 4), local(grad_x, gx_buf, 5), local(grad_y, gy_buf, 6)]
    cps_m = [
        local(first_x, fm.at[:, pl.ds(0, w)], 7),
        local(first_y, fm.at[:, pl.ds(w, w)], 8),
        local(second_x, sm.at[:, pl.ds(0, w)], 9),
        local(second_y, sm.at[:, pl.ds(w, w)], 10),
    ]

    barrier = pltpu.get_barrier_semaphore()
    peers = [{"fs": lax.rem(z + k, nz) * 2 + c} for k in range(1, nz)] + [{"fs": o}]
    peers += [{"tp": lax.rem(t + k, ntp)} for k in range(1, ntp)]
    for dev in peers:
        pl.semaphore_signal(barrier, inc=1, device_id=dev, device_id_type=MESH)
    pl.semaphore_wait(barrier, len(peers))
    for cp in cps_f:
        cp.wait()

    sent = []

    def go(cp):
        cp.start()
        sent.append(cp)

    def piece(src_fs, part):
        return f_buf.at[:, pl.ds(pl.multiple_of(src_fs * R + part * rq, rq), rq)]

    own = piece(i, u)
    for k in range(1, nz):
        zd = lax.rem(z + k, nz)
        go(send(own, own, f_line_s.at[k], f_line_r.at[z], {"fs": zd * 2 + c}))
    mine = f_buf.at[:, rows(i, R)]
    go(send(mine, mine, f_own_s.at[0], f_sib_r.at[z, 0], {"fs": o}))

    for cp in cps_w:
        cp.wait()
    w16[...] = w_buf[...].astype(BF16)
    put = local(w16, w_out.at[rows(i, R)], 2)

    half = R // 2

    def w_hop(step, part):
        for side, sign in ((0, 1), (1, -1)):
            src = z - sign * step
            nxt = z + sign
            has = (src >= 0) & (src < nz)
            to = has & (nxt >= 0) & (nxt < nz)
            slot = w_out.at[rows((src * 2 + c) * 2 + part, half)]

            if step:

                @pl.when(has)
                def _():
                    arrived = w_r.at[src, part]
                    send(slot, slot, w_s.at[0, side, part], arrived, {"fs": o}).wait_recv()

            @pl.when(to)
            def _():
                a = slot if step else w16.at[pl.ds(part * half, half)]
                there = {"fs": nxt * 2 + c}
                send(a, slot, w_s.at[step, side, part], w_r.at[src, part], there).start()

            if step:

                @pl.when(has)
                def _():
                    sib_sems = w_sib_s.at[src, part], w_sib_r.at[src, part]
                    send(slot, slot, *sib_sems, {"fs": o}).start()

    def w_at(point):
        for step, part in PLACE.get(point, ()):
            if step == "rest":
                for k in range(part, nz):
                    w_hop(k, 0)
                    w_hop(k, 1)
            elif step < nz:
                w_hop(step, part)

    w_hop(0, 0)
    w_hop(0, 1)
    for part in range(2):
        a, b = w16.at[pl.ds(part * half, half)], w_out.at[rows(i * 2 + part, half)]
        go(send(a, b, w_sib_s.at[z, part], w_sib_r.at[z, part], {"fs": o}))

    for k in range(1, nz):
        zs = lax.rem(z + nz - k, nz)
        p = piece(zs * 2 + c, u)
        send(p, p, f_line_s.at[k], f_line_r.at[zs], {"fs": o}).wait_recv()
        for v in range(1, q):
            go(send(p, p, f_tp_s.at[zs, v], f_tp_r.at[zs, u], {"tp": g0 + lax.rem(u + v, q)}))
        go(send(p, p, f_sib_s.at[zs, 0], f_sib_r.at[zs, u], {"fs": o}))
    for k in range(1, nz):
        zs = lax.rem(z + nz - k, nz)
        for v in range(1, q):
            part = lax.rem(u + v, q)
            p = piece(zs * 2 + c, part)
            send(p, p, f_tp_s.at[zs, v], f_tp_r.at[zs, part], {"fs": o}).wait_recv()
            go(send(p, p, f_sib_s.at[zs, v], f_sib_r.at[zs, part], {"fs": o}))
    theirs = f_buf.at[:, rows(o, R)]
    send(theirs, theirs, f_own_s.at[0], f_sib_r.at[z, 0], {"fs": o}).wait_recv()
    for k in range(1, nz):
        zs = lax.rem(z + nz - k, nz)
        for v in range(q):
            p = piece(zs * 2 + 1 - c, v)
            send(p, p, f_sib_s.at[zs, v], f_sib_r.at[zs, v], {"fs": o}).wait_recv()

    w_at("factors")
    for cp in cps_n:
        cp.wait()
    tile = min(256, tokens)

    @pl.loop(0, tokens // tile)
    def _(k):
        a = n_buf[rows(k, tile), :]
        for b in range(2):
            h = jnp.dot(a, f_buf[b], preferred_element_type=F32)
            h_buf[rows(k, tile), pl.ds(b * rank, rank)] = h.astype(BF16)

    w_at("h")
    lanes = 128
    m = lanes // (2 * r)

    @pl.loop(0, rank // lanes)
    def _(k):
        for b, g in ((0, gx_buf), (1, gy_buf)):
            h = h_buf[:, pl.ds(pl.multiple_of(b * rank + k * lanes, lanes), lanes)]
            part = lax.dot_general(h, g[...], ROWS, preferred_element_type=F32)
            low[pl.ds(k * m, m), :, :, pl.ds(b * w, w)] = part.reshape(m, 2, r, w)

    w_at("low")
    go(send(low.at[:, 1 - c], sib, sib_s.at[0], sib_s.at[1], {"fs": o}))
    sent[-1].wait_recv()
    for k in range(1, nz):
        zd = lax.rem(z + k, nz)
        rs_send[zd] = (low[zd, c] + sib[zd]).astype(BF16)
        go(send(rs_send.at[zd], rs_recv.at[z], rs_s.at[k], rs_r.at[z], {"fs": zd * 2 + c}))

    w_at("scatter")

    @pl.loop(0, rank // lanes)
    def _(k):
        for b in range(2):
            cols = pl.ds(pl.multiple_of(k * lanes, lanes), lanes)
            gram = lax.dot_general(f_buf[b, :, cols], f_buf[b], ROWS, preferred_element_type=F32)
            hi = gram.astype(BF16)
            g_hi[b, rows(k, lanes), :] = hi
            g_lo[b, rows(k, lanes), :] = (gram - hi.astype(F32)).astype(BF16)

    w_at("gram")
    for cp in cps_m:
        cp.wait()
    total = low[z, c] + sib[z]
    for k in range(1, nz):
        zs = lax.rem(z + k, nz)
        send(rs_recv.at[zs], rs_recv.at[zs], rs_s.at[k], rs_r.at[zs], {"fs": o}).wait_recv()
        total = total + rs_recv[zs].astype(F32)
    low_out[...] = total
    nf = 0.8 * fm[...] + 0.2 * total
    ns = 0.9 * sm[...] + 0.1 * total * total
    d_buf[rows(i, r), :] = (nf / jnp.sqrt(ns)).astype(BF16)

    w_at("predir")
    d_own = d_buf.at[rows(i, r)]
    for k in range(1, nz):
        zd = lax.rem(z + k, nz)
        go(send(d_own, d_own, d_line_s.at[k], d_line_r.at[z], {"fs": zd * 2 + c}))
    go(send(d_own, d_own, d_sib_s.at[z], d_sib_r.at[z], {"fs": o}))
    w_at("dir")
    for k in range(1, nz):
        zs = lax.rem(z + k, nz)
        p = d_buf.at[rows(zs * 2 + c, r)]
        send(p, p, d_line_s.at[k], d_line_r.at[zs], {"fs": o}).wait_recv()
        go(send(p, p, d_sib_s.at[zs], d_sib_r.at[zs], {"fs": o}))
    for k in range(nz):
        zs = lax.rem(z + k, nz)
        p = d_buf.at[rows(zs * 2 + 1 - c, r)]
        send(p, p, d_sib_s.at[zs], d_sib_r.at[zs], {"fs": o}).wait_recv()

    w_at("gathered")
    part = 0.0
    for b in range(2):
        d = d_buf[:, pl.ds(b * w, w)]
        gd = jnp.dot(g_hi[b], d, preferred_element_type=F32)
        gd = gd + jnp.dot(g_lo[b], d, preferred_element_type=F32)
        part = part + jnp.sum(gd * d.astype(F32))
    tot_recv[t] = jnp.full(tot_recv.shape[1:], part, F32)
    for k in range(1, ntp):
        slot = tot_recv.at[t]
        go(send(slot, slot, t_s.at[k], t_r.at[t], {"tp": lax.rem(t + k, ntp)}))

    w_at("end")

    acc = tot_recv[t]
    for k in range(1, ntp):
        ts = lax.rem(t + k, ntp)
        slot = tot_recv.at[ts]
        send(slot, slot, t_s.at[k], t_r.at[ts], {"fs": o}).wait_recv()
        acc = acc + tot_recv[ts]
    tot_out[...] = acc

    for part in range(2):
        for zs in range(nz):
            slot = w_out.at[pl.ds(zs * 2 * R, half)]
            done = send(slot, slot, w_sib_s.at[zs, part], w_sib_r.at[zs, part], {"fs": o})
            done.wait_recv()

            @pl.when(zs != z)
            def _():
                done.wait_send()

        for step in range(nz - 1):
            for side, sign in ((0, 1), (1, -1)):
                src = z - sign * step
                nxt = z + sign

                @pl.when((src >= 0) & (src < nz) & (nxt >= 0) & (nxt < nz))
                def _():
                    a = w16.at[pl.ds(0, half)]
                    send(a, a, w_s.at[step, side, part], w_r.at[0, part], {"fs": o}).wait_send()

    for cp in sent:
        cp.wait_send()
    put.wait()


def output_kernel(
    scale_top,
    f_full,
    w_full,
    d,
    low,
    tot,
    weight_x,
    weight_y,
    factor_x,
    factor_y,
    first_x,
    first_y,
    second_x,
    second_y,
    new_x,
    new_y,
    step_x,
    step_y,
    nf_x,
    nf_y,
    ns_x,
    ns_y,
    copy_x,
    copy_y,
):
    scale = jnp.minimum(1.0, scale_top / jnp.sqrt(tot[0:1, 0:1]))
    w = weight_x.shape[1]
    sides = (
        (factor_x, weight_x, first_x, second_x, new_x, step_x, nf_x, ns_x, copy_x),
        (factor_y, weight_y, first_y, second_y, new_y, step_y, nf_y, ns_y, copy_y),
    )
    for b, (factor, weight, first, second, new, step, nf, ns, copy) in enumerate(sides):
        cols = pl.ds(b * w, w)
        db = d[:, cols]
        up = jnp.dot(f_full[b], db, preferred_element_type=F32)
        copy[...] = (w_full[:, cols].astype(F32) - 0.02 * (scale * up)).astype(BF16)
        st = scale * jnp.dot(factor[...], db, preferred_element_type=F32)
        step[...] = st
        new[...] = weight[...] - 0.02 * st

        @pl.when(pl.program_id(0) == 0)
        def _():
            lo = low[:, cols]
            nf[...] = 0.8 * first[...] + 0.2 * lo
            ns[...] = 0.9 * second[...] + 0.1 * lo * lo


def on_device(nfs, ntp, normed, gx, gy, wx, wy, fx, fy, mx, my, sx, sy):
    tokens, depth = normed.shape
    w = gx.shape[1]
    R, rank = fx.shape
    r = rank // nfs
    nz = nfs // 2
    q = math.gcd(ntp, R // 16)
    anyspec = pl.BlockSpec(memory_space=pl.ANY)
    vmem = pl.BlockSpec(memory_space=pltpu.VMEM)
    dma = pltpu.SemaphoreType.DMA
    sds = jax.ShapeDtypeStruct
    V = pltpu.VMEM
    f_full, w_full, d, low, tot = pl.pallas_call(
        functools.partial(exchange_kernel, nfs, ntp),
        out_shape=(
            V((2, depth, rank), BF16),
            V((depth, 2 * w), BF16),
            V((rank, 2 * w), BF16),
            V((r, 2 * w), F32),
            V((8, 128), F32),
        ),
        in_specs=[anyspec] * 11,
        out_specs=(vmem,) * 5,
        scratch_shapes=[
            V((tokens, depth), BF16),
            V((tokens, w), BF16),
            V((tokens, w), BF16),
            V((tokens, 2 * rank), BF16),
            V((nz, 2, r, 2 * w), F32),
            V((nz, r, 2 * w), F32),
            V((nz, r, 2 * w), BF16),
            V((nz, r, 2 * w), BF16),
            V((R, 2 * w), F32),
            V((R, 2 * w), BF16),
            V((r, 2 * w), F32),
            V((r, 2 * w), F32),
            V((2, rank, rank), BF16),
            V((2, rank, rank), BF16),
            V((ntp, 8, 128), F32),
            dma((11,)),
            dma((nz,)),
            dma((nz,)),
            dma((nz, q)),
            dma((nz, q)),
            dma((nz, q)),
            dma((nz, q)),
            dma((1,)),
            dma((nz, 2, 2)),
            dma((nz, 2)),
            dma((nz, 2)),
            dma((nz, 2)),
            dma((2,)),
            dma((nz,)),
            dma((nz,)),
            dma((nz,)),
            dma((nz,)),
            dma((nz,)),
            dma((nz,)),
            dma((ntp,)),
            dma((ntp,)),
        ],
        compiler_params=pltpu.CompilerParams(
            collective_id=0, has_side_effects=True, vmem_limit_bytes=48 * 1024 * 1024
        ),
    )(normed, gx, gy, wx, wy, fx, fy, mx, my, sx, sy)

    n = min(8, R // 16)
    big, small = depth // n, R // n

    def block(rows, cols):
        return pl.BlockSpec((rows, cols), lambda k: (k, 0))

    def whole(rows, cols):
        return pl.BlockSpec((rows, cols), lambda k: (0, 0))

    return pl.pallas_call(
        functools.partial(output_kernel, 0.25 * math.sqrt(2.0 * depth * w * ntp)),
        grid=(n,),
        out_shape=[sds((R, w), F32)] * 4 + [sds((r, w), F32)] * 4 + [sds((depth, w), BF16)] * 2,
        in_specs=[
            pl.BlockSpec((2, big, rank), lambda k: (0, k, 0)),
            block(big, 2 * w),
            whole(rank, 2 * w),
            whole(r, 2 * w),
            whole(8, 128),
        ]
        + [block(small, w)] * 2
        + [block(small, rank)] * 2
        + [whole(r, w)] * 4,
        out_specs=[block(small, w)] * 4 + [whole(r, w)] * 4 + [block(big, w)] * 2,
        compiler_params=pltpu.CompilerParams(vmem_limit_bytes=40 * 1024 * 1024),
    )(f_full, w_full, d, low, tot, wx, wy, fx, fy, mx, my, sx, sy)


def solution(mesh):
    row, cut, rep = P("fs", None), P("fs", "tp"), P(None, "tp")
    return jax.shard_map(
        functools.partial(on_device, mesh.shape["fs"], mesh.shape["tp"]),
        mesh=mesh,
        in_specs=(row, cut, cut, cut, cut, row, row, cut, cut, cut, cut),
        out_specs=(cut,) * 8 + (rep, rep),
        check_vma=False,
    )
```

```python
import functools
import math

import jax
import jax.numpy as jnp
from jax import lax
from jax.experimental import pallas as pl
from jax.experimental.pallas import tpu as pltpu
from jax.sharding import PartitionSpec as P

MESH = pl.DeviceIdType.MESH
F32, BF16 = jnp.float32, jnp.bfloat16
PLACE = {"factors": ((1, 0),), "h": ((1, 1),), "scatter": ((2, 0),), "gram": ((2, 1),), "end": (("rest", 3),)}
ROWS = (((0,), (0,)), ((), ()))


def exchange_kernel(
    nfs,
    ntp,
    normed,
    grad_x,
    grad_y,
    weight_x,
    weight_y,
    factor_x,
    factor_y,
    first_x,
    first_y,
    second_x,
    second_y,
    f_buf,
    w_out,
    d_buf,
    low_out,
    tot_out,
    n_buf,
    gx_buf,
    gy_buf,
    h_buf,
    low,
    sib,
    rs_send,
    rs_recv,
    w_buf,
    w16,
    fm,
    sm,
    g_hi,
    g_lo,
    tot_recv,
    lsem,
    f_line_s,
    f_line_r,
    f_tp_s,
    f_tp_r,
    f_sib_s,
    f_sib_r,
    f_own_s,
    w_s,
    w_r,
    w_sib_s,
    w_sib_r,
    sib_s,
    rs_s,
    rs_r,
    d_line_s,
    d_line_r,
    d_sib_s,
    d_sib_r,
    t_s,
    t_r,
):
    nz = nfs // 2
    i = lax.axis_index("fs")
    t = lax.axis_index("tp")
    z, c = i // 2, lax.rem(i, 2)
    o = z * 2 + 1 - c
    R, rank = factor_x.shape
    tokens, w = gx_buf.shape
    r = rank // nfs
    q = math.gcd(ntp, R // 16)
    rq = R // q
    u, g0 = lax.rem(t, q), t // q * q

    def local(src, dst, k):
        cp = pltpu.make_async_copy(src, dst, lsem.at[k])
        cp.start()
        return cp

    def send(src, dst, s, rr, dev):
        return pltpu.make_async_remote_copy(
            src_ref=src, dst_ref=dst, send_sem=s, recv_sem=rr, device_id=dev, device_id_type=MESH
        )

    def rows(k, n):
        return pl.ds(pl.multiple_of(k * n, n), n)

    cps_f = [
        local(factor_x, f_buf.at[0, rows(i, R)], 0),
        local(factor_y, f_buf.at[1, rows(i, R)], 1),
    ]
    cps_w = [
        local(weight_x, w_buf.at[:, pl.ds(0, w)], 2),
        local(weight_y, w_buf.at[:, pl.ds(w, w)], 3),
    ]
    cps_n = [local(normed, n_buf, 4), local(grad_x, gx_buf, 5), local(grad_y, gy_buf, 6)]
    cps_m = [
        local(first_x, fm.at[:, pl.ds(0, w)], 7),
        local(first_y, fm.at[:, pl.ds(w, w)], 8),
        local(second_x, sm.at[:, pl.ds(0, w)], 9),
        local(second_y, sm.at[:, pl.ds(w, w)], 10),
    ]

    barrier = pltpu.get_barrier_semaphore()
    peers = [{"fs": lax.rem(z + k, nz) * 2 + c} for k in range(1, nz)] + [{"fs": o}]
    peers += [{"tp": lax.rem(t + k, ntp)} for k in range(1, ntp)]
    for dev in peers:
        pl.semaphore_signal(barrier, inc=1, device_id=dev, device_id_type=MESH)
    pl.semaphore_wait(barrier, len(peers))
    for cp in cps_f:
        cp.wait()

    sent = []

    def go(cp):
        cp.start()
        sent.append(cp)

    def piece(src_fs, part):
        return f_buf.at[:, pl.ds(pl.multiple_of(src_fs * R + part * rq, rq), rq)]

    own = piece(i, u)
    for k in range(1, nz):
        zd = lax.rem(z + k, nz)
        go(send(own, own, f_line_s.at[k], f_line_r.at[z], {"fs": zd * 2 + c}))
    mine = f_buf.at[:, rows(i, R)]
    go(send(mine, mine, f_own_s.at[0], f_sib_r.at[z, 0], {"fs": o}))

    for cp in cps_w:
        cp.wait()
    w16[...] = w_buf[...].astype(BF16)
    put = local(w16, w_out.at[rows(i, R)], 2)

    half = R // 2

    def w_hop(step, part):
        for side, sign in ((0, 1), (1, -1)):
            src = z - sign * step
            nxt = z + sign
            has = (src >= 0) & (src < nz)
            to = has & (nxt >= 0) & (nxt < nz)
            slot = w_out.at[rows((src * 2 + c) * 2 + part, half)]

            if step:

                @pl.when(has)
                def _():
                    arrived = w_r.at[src, part]
                    send(slot, slot, w_s.at[0, side, part], arrived, {"fs": o}).wait_recv()

            @pl.when(to)
            def _():
                a = slot if step else w16.at[pl.ds(part * half, half)]
                there = {"fs": nxt * 2 + c}
                send(a, slot, w_s.at[step, side, part], w_r.at[src, part], there).start()

            if step:

                @pl.when(has)
                def _():
                    sib_sems = w_sib_s.at[src, part], w_sib_r.at[src, part]
                    send(slot, slot, *sib_sems, {"fs": o}).start()

    def w_at(point):
        for step, part in PLACE.get(point, ()):
            if step == "rest":
                for k in range(part, nz):
                    w_hop(k, 0)
                    w_hop(k, 1)
            elif step < nz:
                w_hop(step, part)

    w_hop(0, 0)
    w_hop(0, 1)
    for part in range(2):
        a, b = w16.at[pl.ds(part * half, half)], w_out.at[rows(i * 2 + part, half)]
        go(send(a, b, w_sib_s.at[z, part], w_sib_r.at[z, part], {"fs": o}))

    for k in range(1, nz):
        zs = lax.rem(z + nz - k, nz)
        p = piece(zs * 2 + c, u)
        send(p, p, f_line_s.at[k], f_line_r.at[zs], {"fs": o}).wait_recv()
        for v in range(1, q):
            go(send(p, p, f_tp_s.at[zs, v], f_tp_r.at[zs, u], {"tp": g0 + lax.rem(u + v, q)}))
        go(send(p, p, f_sib_s.at[zs, 0], f_sib_r.at[zs, u], {"fs": o}))
    for k in range(1, nz):
        zs = lax.rem(z + nz - k, nz)
        for v in range(1, q):
            part = lax.rem(u + v, q)
            p = piece(zs * 2 + c, part)
            send(p, p, f_tp_s.at[zs, v], f_tp_r.at[zs, part], {"fs": o}).wait_recv()
            go(send(p, p, f_sib_s.at[zs, v], f_sib_r.at[zs, part], {"fs": o}))
    theirs = f_buf.at[:, rows(o, R)]
    send(theirs, theirs, f_own_s.at[0], f_sib_r.at[z, 0], {"fs": o}).wait_recv()
    for k in range(1, nz):
        zs = lax.rem(z + nz - k, nz)
        for v in range(q):
            p = piece(zs * 2 + 1 - c, v)
            send(p, p, f_sib_s.at[zs, v], f_sib_r.at[zs, v], {"fs": o}).wait_recv()

    w_at("factors")
    for cp in cps_n:
        cp.wait()
    tile = min(256, tokens)

    @pl.loop(0, tokens // tile)
    def _(k):
        a = n_buf[rows(k, tile), :]
        for b in range(2):
            h = jnp.dot(a, f_buf[b], preferred_element_type=F32)
            h_buf[rows(k, tile), pl.ds(b * rank, rank)] = h.astype(BF16)

    w_at("h")
    lanes = 128
    m = lanes // (2 * r)

    @pl.loop(0, rank // lanes)
    def _(k):
        for b, g in ((0, gx_buf), (1, gy_buf)):
            h = h_buf[:, pl.ds(pl.multiple_of(b * rank + k * lanes, lanes), lanes)]
            part = lax.dot_general(h, g[...], ROWS, preferred_element_type=F32)
            low[pl.ds(k * m, m), :, :, pl.ds(b * w, w)] = part.reshape(m, 2, r, w)

    w_at("low")
    go(send(low.at[:, 1 - c], sib, sib_s.at[0], sib_s.at[1], {"fs": o}))
    sent[-1].wait_recv()
    for k in range(1, nz):
        zd = lax.rem(z + k, nz)
        rs_send[zd] = (low[zd, c] + sib[zd]).astype(BF16)
        go(send(rs_send.at[zd], rs_recv.at[z], rs_s.at[k], rs_r.at[z], {"fs": zd * 2 + c}))

    w_at("scatter")

    @pl.loop(0, rank // lanes)
    def _(k):
        for b in range(2):
            cols = pl.ds(pl.multiple_of(k * lanes, lanes), lanes)
            gram = lax.dot_general(f_buf[b, :, cols], f_buf[b], ROWS, preferred_element_type=F32)
            hi = gram.astype(BF16)
            g_hi[b, rows(k, lanes), :] = hi
            g_lo[b, rows(k, lanes), :] = (gram - hi.astype(F32)).astype(BF16)

    w_at("gram")
    for cp in cps_m:
        cp.wait()
    total = low[z, c] + sib[z]
    for k in range(1, nz):
        zs = lax.rem(z + k, nz)
        send(rs_recv.at[zs], rs_recv.at[zs], rs_s.at[k], rs_r.at[zs], {"fs": o}).wait_recv()
        total = total + rs_recv[zs].astype(F32)
    low_out[...] = total
    nf = 0.8 * fm[...] + 0.2 * total
    ns = 0.9 * sm[...] + 0.1 * total * total
    d_buf[rows(i, r), :] = (nf / jnp.sqrt(ns)).astype(BF16)

    w_at("predir")
    d_own = d_buf.at[rows(i, r)]
    for k in range(1, nz):
        zd = lax.rem(z + k, nz)
        go(send(d_own, d_own, d_line_s.at[k], d_line_r.at[z], {"fs": zd * 2 + c}))
    go(send(d_own, d_own, d_sib_s.at[z], d_sib_r.at[z], {"fs": o}))
    w_at("dir")
    for k in range(1, nz):
        zs = lax.rem(z + k, nz)
        p = d_buf.at[rows(zs * 2 + c, r)]
        send(p, p, d_line_s.at[k], d_line_r.at[zs], {"fs": o}).wait_recv()
        go(send(p, p, d_sib_s.at[zs], d_sib_r.at[zs], {"fs": o}))
    for k in range(nz):
        zs = lax.rem(z + k, nz)
        p = d_buf.at[rows(zs * 2 + 1 - c, r)]
        send(p, p, d_sib_s.at[zs], d_sib_r.at[zs], {"fs": o}).wait_recv()

    w_at("gathered")
    part = 0.0
    for b in range(2):
        d = d_buf[:, pl.ds(b * w, w)]
        gd = jnp.dot(g_hi[b], d, preferred_element_type=F32)
        gd = gd + jnp.dot(g_lo[b], d, preferred_element_type=F32)
        part = part + jnp.sum(gd * d.astype(F32))
    tot_recv[t] = jnp.full(tot_recv.shape[1:], part, F32)
    for k in range(1, ntp):
        slot = tot_recv.at[t]
        go(send(slot, slot, t_s.at[k], t_r.at[t], {"tp": lax.rem(t + k, ntp)}))

    w_at("end")

    acc = tot_recv[t]
    for k in range(1, ntp):
        ts = lax.rem(t + k, ntp)
        slot = tot_recv.at[ts]
        send(slot, slot, t_s.at[k], t_r.at[ts], {"fs": o}).wait_recv()
        acc = acc + tot_recv[ts]
    tot_out[...] = acc

    for part in range(2):
        for zs in range(nz):
            slot = w_out.at[pl.ds(zs * 2 * R, half)]
            done = send(slot, slot, w_sib_s.at[zs, part], w_sib_r.at[zs, part], {"fs": o})
            done.wait_recv()

            @pl.when(zs != z)
            def _():
                done.wait_send()

        for step in range(nz - 1):
            for side, sign in ((0, 1), (1, -1)):
                src = z - sign * step
                nxt = z + sign

                @pl.when((src >= 0) & (src < nz) & (nxt >= 0) & (nxt < nz))
                def _():
                    a = w16.at[pl.ds(0, half)]
                    send(a, a, w_s.at[step, side, part], w_r.at[0, part], {"fs": o}).wait_send()

    for cp in sent:
        cp.wait_send()
    put.wait()


def output_kernel(
    scale_top,
    f_full,
    w_full,
    d,
    low,
    tot,
    weight_x,
    weight_y,
    factor_x,
    factor_y,
    first_x,
    first_y,
    second_x,
    second_y,
    new_x,
    new_y,
    step_x,
    step_y,
    nf_x,
    nf_y,
    ns_x,
    ns_y,
    copy_x,
    copy_y,
):
    scale = jnp.minimum(1.0, scale_top / jnp.sqrt(tot[0:1, 0:1]))
    w = weight_x.shape[1]
    big = copy_x.shape[0]
    now = pl.ds(pl.multiple_of(pl.program_id(0) * big, big), big)
    sides = (
        (factor_x, weight_x, first_x, second_x, new_x, step_x, nf_x, ns_x, copy_x),
        (factor_y, weight_y, first_y, second_y, new_y, step_y, nf_y, ns_y, copy_y),
    )
    for b, (factor, weight, first, second, new, step, nf, ns, copy) in enumerate(sides):
        cols = pl.ds(b * w, w)
        db = d[:, cols]
        up = jnp.dot(f_full[b, now, :], db, preferred_element_type=F32)
        copy[...] = (w_full[now, cols].astype(F32) - 0.02 * (scale * up)).astype(BF16)
        st = scale * jnp.dot(factor[...], db, preferred_element_type=F32)
        step[...] = st
        new[...] = weight[...] - 0.02 * st

        @pl.when(pl.program_id(0) == 0)
        def _():
            lo = low[:, cols]
            nf[...] = 0.8 * first[...] + 0.2 * lo
            ns[...] = 0.9 * second[...] + 0.1 * lo * lo


def on_device(nfs, ntp, normed, gx, gy, wx, wy, fx, fy, mx, my, sx, sy):
    tokens, depth = normed.shape
    w = gx.shape[1]
    R, rank = fx.shape
    r = rank // nfs
    nz = nfs // 2
    q = math.gcd(ntp, R // 16)
    anyspec = pl.BlockSpec(memory_space=pl.ANY)
    vmem = pl.BlockSpec(memory_space=pltpu.VMEM)
    dma = pltpu.SemaphoreType.DMA
    sds = jax.ShapeDtypeStruct
    V = pltpu.VMEM
    f_full, w_full, d, low, tot = pl.pallas_call(
        functools.partial(exchange_kernel, nfs, ntp),
        out_shape=(
            V((2, depth, rank), BF16),
            V((depth, 2 * w), BF16),
            V((rank, 2 * w), BF16),
            V((r, 2 * w), F32),
            V((8, 128), F32),
        ),
        in_specs=[anyspec] * 11,
        out_specs=(vmem,) * 5,
        scratch_shapes=[
            V((tokens, depth), BF16),
            V((tokens, w), BF16),
            V((tokens, w), BF16),
            V((tokens, 2 * rank), BF16),
            V((nz, 2, r, 2 * w), F32),
            V((nz, r, 2 * w), F32),
            V((nz, r, 2 * w), BF16),
            V((nz, r, 2 * w), BF16),
            V((R, 2 * w), F32),
            V((R, 2 * w), BF16),
            V((r, 2 * w), F32),
            V((r, 2 * w), F32),
            V((2, rank, rank), BF16),
            V((2, rank, rank), BF16),
            V((ntp, 8, 128), F32),
            dma((11,)),
            dma((nz,)),
            dma((nz,)),
            dma((nz, q)),
            dma((nz, q)),
            dma((nz, q)),
            dma((nz, q)),
            dma((1,)),
            dma((nz, 2, 2)),
            dma((nz, 2)),
            dma((nz, 2)),
            dma((nz, 2)),
            dma((2,)),
            dma((nz,)),
            dma((nz,)),
            dma((nz,)),
            dma((nz,)),
            dma((nz,)),
            dma((nz,)),
            dma((ntp,)),
            dma((ntp,)),
        ],
        compiler_params=pltpu.CompilerParams(
            collective_id=0, has_side_effects=True, vmem_limit_bytes=48 * 1024 * 1024
        ),
    )(normed, gx, gy, wx, wy, fx, fy, mx, my, sx, sy)

    n = min(4, R // 16)
    big, small = depth // n, R // n

    def block(rows, cols):
        return pl.BlockSpec((rows, cols), lambda k: (k, 0))

    def whole(rows, cols):
        return pl.BlockSpec((rows, cols), lambda k: (0, 0))

    return pl.pallas_call(
        functools.partial(output_kernel, 0.25 * math.sqrt(2.0 * depth * w * ntp)),
        grid=(n,),
        out_shape=[sds((R, w), F32)] * 4 + [sds((r, w), F32)] * 4 + [sds((depth, w), BF16)] * 2,
        in_specs=[
            vmem,
            vmem,
            vmem,
            whole(r, 2 * w),
            whole(8, 128),
        ]
        + [block(small, w)] * 2
        + [block(small, rank)] * 2
        + [whole(r, w)] * 4,
        out_specs=[block(small, w)] * 4 + [whole(r, w)] * 4 + [block(big, w)] * 2,
        compiler_params=pltpu.CompilerParams(vmem_limit_bytes=40 * 1024 * 1024),
    )(f_full, w_full, d, low, tot, wx, wy, fx, fy, mx, my, sx, sy)


def solution(mesh):
    row, cut, rep = P("fs", None), P("fs", "tp"), P(None, "tp")
    return jax.shard_map(
        functools.partial(on_device, mesh.shape["fs"], mesh.shape["tp"]),
        mesh=mesh,
        in_specs=(row, cut, cut, cut, cut, row, row, cut, cut, cut, cut),
        out_specs=(cut,) * 8 + (rep, rep),
        check_vma=False,
    )
```
